256 devices in a mesh: ep: 64 (over z, x, core), tp: 4 (over y).
Axes of the slice: x: 4, y: 4, z: 8, core: 2. Of those that a mesh axis runs over, the one named last changes fastest.
Arguments:
- pool_input: bfloat16 [32768, 1024], P('ep', 'tp'), may hold values from -6 to 6
- group_weight: bfloat16 [4, 256, 256], P('tp'), may hold values from -0.375 to 0.375
- pool_scale: float32 [1024], P('tp'), may hold values from 0.1 to 1.9
- out_weight: bfloat16 [1024, 2048], P('tp'), may hold values from -0.1875 to 0.1875
- mix_gain: float32 [2048], replicated, may hold values from 0.1 to 1.9
- expert_input: bfloat16 [65536, 2048], P(('ep', 'tp')), may hold values from -6 to 6
- routes: int32 [65536, 2], P('ep'), may hold values from 0 to 127, all different within a row; in each aligned block of 256 rows (0 to 255, 256 to 511, ...) at most 5 rows name the same one
- route_weights: float32 [65536, 2], P('ep'), may hold values from 0.2 to 2.5
- moe_in_gain: float32 [2048], replicated, may hold values from 0.1 to 1.9
- gate_weight: bfloat16 [128, 2048, 1024], P('ep', None, 'tp'), may hold values from -0.125 to 0.125
- up_weight: bfloat16 [128, 2048, 1024], P('ep', None, 'tp'), may hold values from -0.125 to 0.125
- down_weight: bfloat16 [128, 1024, 2048], P('ep', 'tp'), may hold values from -0.1875 to 0.1875
- moe_out_gain: float32 [2048], replicated, may hold values from 0.1 to 1.9
Outputs:
- mixer_out: bfloat16 [32768, 2048], P(('ep', 'tp'))
- moe_out: bfloat16 [65536, 2048], P(('ep', 'tp'))
The draws below stay inside these ranges and needn't reach their ends.
Inputs may be any that keep to these rules, and one draw needn't show every extreme that they name: `routes`: each row names 2 different experts. In each aligned block of 256 rows no expert is named by more than 5 rows, a bound that some block reaches.
All inputs are finite; a program needn't handle non-finite values.
Results may differ from the reference program's by a relative error of at most 0.013.
Values may be sent and summed in bfloat16 or wider, within the bound.
No kernel may reach another device: no remote copies, remote signals or barrier semaphores. Data moves between devices by JAX's collectives and lax.ppermute only.
A program may use at most 128 MiB of HBM per device.

```python
import math
from functools import partial
import jax
import jax.numpy as jnp
import numpy as np
from jax import lax

D = 2048
GROUPS = 4
GW = 256
PW = 1024
FF = 1024
FF_BLK = 256
EXPERTS = 128
TOPK = 2
TOKB_DEV = 256
CAP = 5
TOKENS_A = 32768
TOKENS_B = 65536
N_TP = 4


def block_levels(key, shape, shards, smallest, high):
    gain, own = 1.0, jax.random.fold_in(key, 6)
    for dim, blocks in shards:
        steps = jnp.exp(jax.random.uniform(jax.random.fold_in(own, dim), (blocks,), jnp.float32, smallest / len(shards), high / len(shards)))
        gain = gain * jnp.repeat(steps, shape[dim] // blocks).reshape([-1 if axis == dim else 1 for axis in range(len(shape))])
    return gain


def deal_out(key, own, number, rows, number_of, top, most, slope):
    ranking = jax.random.permutation(key, number_of)
    crowded, usual = shares(number_of, rows * top, most, slope, True), shares(number_of, rows * top, most, slope, False)
    places = jnp.arange(number_of)

    def named(sizes, rotation):
        used = int((sizes > 0).sum())
        fixed = max(1, used // 4)
        passed = fixed + (places - fixed + rotation * (used - fixed)) % max(1, number_of - fixed)
        return jnp.zeros((number_of,), jnp.int32).at[ranking[jnp.where(places < fixed, places, passed)]].set(jnp.asarray(sizes, jnp.int32))

    sizes = jnp.where(number % 4 == 0, named(crowded, number // 4), named(usual, number - number // 4 - 1))
    mixed = jax.random.permutation(jax.random.fold_in(own, 3), number_of)
    donor, sink = mixed[0:number_of // 2 * 2:2], mixed[1:number_of // 2 * 2:2]
    margin = jnp.minimum(sizes[donor] - 1, most - sizes[sink]) // 2
    margin = jnp.where((donor == ranking[0]) | (sink == ranking[0]) | (sizes[sink] == 0), 0, jnp.maximum(margin, 0))
    passed = jax.random.randint(jax.random.fold_in(own, 4), (number_of // 2,), 0, 1 << 20) % (margin + 1)
    sizes = sizes.at[donor].add(-passed).at[sink].add(passed)
    items = jnp.searchsorted(jnp.cumsum(sizes), jnp.arange(rows * top), side="right").astype(jnp.int32)
    grid = items.reshape(top, rows).T
    grid = grid[jax.random.permutation(jax.random.fold_in(own, 1), rows)]
    rotation = jax.random.randint(jax.random.fold_in(own, 2), (rows, 1), 0, top)
    return jnp.take_along_axis(grid, (jnp.arange(top)[None, :] + rotation) % top, axis=1)


def shares(number_of, total, bound, skew, full):
    portions = [(1 << 20) // math.isqrt(rank ** skew) + 1 for rank in range(1, number_of + 1)]
    largest = bound if full else min(bound, max(-(-total // number_of), total * portions[0] // sum(portions)))
    least = 1 if total - largest >= number_of - 1 else 0
    given, rest = [largest] + [least] * (number_of - 1), total - largest - least * (number_of - 1)
    while rest > 0:
        movable = [i for i in range(1, number_of) if given[i] < largest] or [i for i in range(1, number_of) if given[i] < bound]
        whole, remaining = sum([portions[i] for i in movable]), rest
        for i in movable:
            more = min(bound - given[i], max(1, remaining * portions[i] // whole), rest)
            given[i] = given[i] + more
            rest = rest - more
    return np.array(given)


def scatter_about(own_key, dims, scale, bound, split=(), kind=jnp.bfloat16):
    entries = scale * jax.random.normal(own_key, dims, jnp.float32)
    if split:
        entries = entries * block_levels(own_key, dims, split, -0.22, 0.18)
    return jnp.clip(entries, -bound, bound).astype(kind)


def setup_inputs(seed: int = 0) -> dict:
    key_list = jax.random.split(jax.random.key(seed), 14)
    pool_input = scatter_about(key_list[0], (TOKENS_A, PW), 1.0, 6.0, ((0, 64), (1, 4)))
    group_weight = scatter_about(key_list[1], (GROUPS, GW, GW), GW ** -0.5, 0.375, ((0, 4),))
    pool_scale = jnp.clip(1.0 + 0.18 * jax.random.normal(key_list[2], (PW,), jnp.float32), 0.1, 1.9)
    out_weight = scatter_about(key_list[3], (PW, D), PW ** -0.5, 0.1875, ((0, 4),))
    mix_gain = jnp.clip(1.0 + 0.18 * jax.random.normal(key_list[4], (D,), jnp.float32), 0.1, 1.9)
    expert_input = scatter_about(key_list[5], (TOKENS_B, D), 1.0, 6.0, ((0, 256),))
    routes_keys = jax.random.split(jax.random.fold_in(key_list[6], 1), TOKENS_B // TOKB_DEV)
    routes_turns = jax.random.permutation(jax.random.fold_in(key_list[6], 3), TOKENS_B // TOKB_DEV)
    routes = jax.vmap(lambda own, number: deal_out(jax.random.fold_in(key_list[6], 2), own, number, TOKB_DEV, EXPERTS, TOPK, CAP, 1))(routes_keys, routes_turns).reshape((TOKENS_B, TOPK))
    route_weights = jnp.clip(jnp.exp(math.log(2.5) - 2.5257286 * jax.random.uniform(key_list[7], (TOKENS_B, TOPK), jnp.float32) ** block_levels(key_list[7], (TOKENS_B, TOPK), ((0, 64),), -0.2, 0.2)), 0.2, 2.5)
    moe_in_gain = jnp.clip(1.0 + 0.18 * jax.random.normal(key_list[8], (D,), jnp.float32), 0.1, 1.9)
    gate_weight = scatter_about(key_list[9], (EXPERTS, D, FF), D ** -0.5, 0.125, ((0, 64), (2, 4)))
    up_weight = scatter_about(key_list[10], (EXPERTS, D, FF), D ** -0.5, 0.125, ((0, 64), (2, 4)))
    down_weight = scatter_about(key_list[11], (EXPERTS, FF, D), FF ** -0.5, 0.1875, ((0, 64), (1, 4)))
    moe_out_gain = jnp.clip(1.0 + 0.18 * jax.random.normal(key_list[12], (D,), jnp.float32), 0.1, 1.9)
    return {"pool_input": pool_input, "group_weight": group_weight, "pool_scale": pool_scale, "out_weight": out_weight, "mix_gain": mix_gain, "expert_input": expert_input, "routes": routes, "route_weights": route_weights, "moe_in_gain": moe_in_gain, "gate_weight": gate_weight, "up_weight": up_weight, "down_weight": down_weight, "moe_out_gain": moe_out_gain}


NORM_EPS = 1e-06

def rms_scale(values, gain_vec):
    mean_sq = lax.optimization_barrier(jnp.mean(values * values, axis=-1, keepdims=True))
    return values * lax.rsqrt(mean_sq + NORM_EPS) * gain_vec.astype(jnp.float32)

def pool_group(block_in, window):
    row_total = block_in.shape[0]
    values = block_in.astype(jnp.float32)
    padded = jnp.pad(values, ((window - 1, 0), (0, 0)))
    summed = jnp.zeros_like(values)
    for lag_step in range(window):
        summed = summed + padded[window - 1 - lag_step:window - 1 - lag_step + row_total]
    divisor = jnp.minimum(jnp.arange(row_total) + 1, window).astype(jnp.float32)[:, None]
    return (summed / divisor - values).astype(jnp.bfloat16)

def slot_numbers(route_block, experts, capacity):
    flat_routes = route_block.reshape(-1).astype(jnp.int32)
    one_hot = (flat_routes[:, None] == jnp.arange(experts, dtype=jnp.int32)[None, :]).astype(jnp.int32)
    slot_rank = lax.optimization_barrier(jnp.sum((jnp.cumsum(one_hot, axis=0) - one_hot) * one_hot, axis=1))
    return (flat_routes * capacity + slot_rank).astype(jnp.int32)

def fill_table(slot_ids, payload, empty_value, slots_total):
    return jnp.full((slots_total,), empty_value, payload.dtype).at[slot_ids].set(payload)

def reference(pool_input, group_weight, pool_scale, out_weight, mix_gain, expert_input, routes, route_weights, moe_in_gain, gate_weight, up_weight, down_weight, moe_out_gain):
    projected = jnp.zeros((TOKENS_A, D), jnp.float32)
    for group_idx in range(GROUPS):
        lo_col = group_idx * GW
        pooled = pool_group(pool_input[:, lo_col:lo_col + GW], 2 ** (group_idx + 1))
        grouped = (jnp.dot(pooled, group_weight[group_idx], preferred_element_type=jnp.float32) * pool_scale[lo_col:lo_col + GW].astype(jnp.float32)).astype(jnp.bfloat16)
        partial_mix = jnp.dot(grouped, out_weight[lo_col:lo_col + GW], preferred_element_type=jnp.float32).astype(jnp.bfloat16)
        projected = projected + partial_mix.astype(jnp.float32)
    mixer_out = rms_scale(projected, mix_gain).astype(jnp.bfloat16)
    normed = rms_scale(expert_input.astype(jnp.float32), moe_in_gain).astype(jnp.bfloat16)
    blocks = TOKENS_B // TOKB_DEV
    pairs = TOKB_DEV * TOPK
    route_blocks = routes.reshape(blocks, TOKB_DEV, TOPK)
    slot_ids = jax.vmap(partial(slot_numbers, experts=EXPERTS, capacity=CAP))(route_blocks)
    pair_token = (jnp.arange(blocks, dtype=jnp.int32)[:, None] * TOKB_DEV + jnp.arange(pairs, dtype=jnp.int32)[None, :] // TOPK).astype(jnp.int32)
    token_table = jax.vmap(partial(fill_table, empty_value=TOKENS_B, slots_total=EXPERTS * CAP))(slot_ids, pair_token)
    weight_table = jax.vmap(partial(fill_table, empty_value=0.0, slots_total=EXPERTS * CAP))(slot_ids, route_weights.reshape(blocks, pairs))
    token_table = token_table.reshape(blocks, EXPERTS, CAP).transpose(1, 0, 2).reshape(EXPERTS, blocks * CAP)
    weight_table = weight_table.reshape(blocks, EXPERTS, CAP).transpose(1, 0, 2).reshape(EXPERTS, blocks * CAP)
    padded_rows = jnp.concatenate([normed, jnp.zeros((1, D), jnp.bfloat16)], axis=0)

    def run_expert(combined, expert_inputs):
        token_idx, slot_weight, w_gate, w_up, w_down = expert_inputs
        gathered = padded_rows[token_idx]
        gate_act = jnp.dot(gathered, w_gate, preferred_element_type=jnp.float32)
        up_act = jnp.dot(gathered, w_up, preferred_element_type=jnp.float32)
        hidden = (jax.nn.silu(gate_act) * up_act).astype(jnp.bfloat16)
        block_parts = jnp.einsum('rjf,jfd->jrd', hidden.reshape(-1, N_TP, FF_BLK).astype(jnp.float32), w_down.reshape(N_TP, FF_BLK, D).astype(jnp.float32)).astype(jnp.bfloat16)
        expert_out = lax.optimization_barrier(jnp.sum(block_parts.astype(jnp.float32), axis=0)).astype(jnp.bfloat16)
        combined = combined.at[token_idx].add(slot_weight[:, None] * expert_out.astype(jnp.float32))
        return (combined, None)
    start_sums = jnp.zeros((TOKENS_B + 1, D), jnp.float32)
    combined, ignored = lax.scan(run_expert, start_sums, (token_table, weight_table, gate_weight, up_weight, down_weight))
    moe_out = rms_scale(combined[:TOKENS_B], moe_out_gain).astype(jnp.bfloat16)
    return (mixer_out, moe_out)
```

```python
import jax
import jax.numpy as jnp
from jax import lax
from jax.sharding import PartitionSpec as P

NORM_EPS = 1e-06

NZ, NX, NC, NT = 8, 4, 2, 4
CAP = 5
MSG = NX * NC * CAP
CHUNK = NZ * MSG
BF = jnp.bfloat16
F32 = jnp.float32


def ep_shift(value, sz, sx, sc):
    pairs = []
    for z in range(NZ):
        for x in range(NX):
            for c in range(NC):
                target = ((z + sz) % NZ * NX + (x + sx) % NX) * NC + (c + sc) % NC
                pairs.append(((z * NX + x) * NC + c, target))
    if all(a == b for a, b in pairs):
        return value
    return lax.ppermute(value, "ep", pairs)


def z_shift(value, sz, hop):
    if not hop:
        return ep_shift(value, sz, 0, 0)
    pairs = []
    plane = NX * NC
    for z in range(NZ):
        for q in range(plane):
            for t in range(NT):
                source = (z * plane + q) * NT + t
                pairs.append((source, ((z + sz) % NZ * plane + q) * NT + (NT - 1 - t)))
    return lax.ppermute(value, ("ep", "tp"), pairs)


def pair_swap(value):
    return lax.ppermute(value, "tp", [(t, t ^ 1) for t in range(NT)])


def cross_swap(value):
    return lax.ppermute(value, "tp", [(t, NT - 1 - t) for t in range(NT)])


def rms_scale(values, gain_vec):
    mean_sq = jnp.mean(values * values, axis=-1, keepdims=True)
    return values * lax.rsqrt(mean_sq + NORM_EPS) * gain_vec


def dot32(a, b):
    return jnp.dot(a, b, preferred_element_type=F32)


def perm_iota():
    i = lax.broadcasted_iota(jnp.int32, (CHUNK, CHUNK), 0)
    j = lax.broadcasted_iota(jnp.int32, (CHUNK, CHUNK), 1)
    q = i // CAP
    source = (q % NZ * NZ + q // NZ) * CAP + i % CAP
    return (j == source).astype(BF)


def mixer_start(pool_input, group_weight, pool_scale, out_weight, ep, tp):
    rows = pool_input.shape[0]
    hist = 2**NT
    quarter = rows // NT
    window = jnp.left_shift(jnp.int32(2), tp)
    history = lax.ppermute(pool_input[rows - hist :], "ep", [(e, e + 1) for e in range(NZ * NX * NC - 1)])
    extended = jnp.concatenate([history, pool_input], axis=0)
    block = lax.broadcasted_iota(jnp.int32, (rows, 1), 0) // quarter
    owner = jnp.where(block % 2 == 0, 0, 3) ^ jnp.where(block // 2 == 0, 0, 1) ^ tp
    place = owner * quarter + lax.broadcasted_iota(jnp.int32, (rows, 1), 0) % quarter
    source = lax.broadcasted_iota(jnp.int32, (rows, rows + hist), 1) - hist
    band = ((source <= place) & (source > place - window)).astype(BF)
    pick = (source == place).astype(BF)
    divisor = jnp.minimum(ep * rows + place + 1, window).astype(F32)
    pooled = (dot32(band, extended) / divisor - dot32(pick, extended)).astype(BF)
    grouped = (dot32(pooled, group_weight[0]) * pool_scale).astype(BF)
    return dot32(grouped, out_weight).astype(BF)


def experts_on(rows, gates, ups, downs):
    total = None
    for gate, up, down in zip(gates, ups, downs):
        hidden = (jax.nn.silu(dot32(rows, gate)) * dot32(rows, up)).astype(BF)
        part = dot32(hidden, down)
        total = part if total is None else total + part
    return total.astype(BF)


def on_device(
    pool_input,
    group_weight,
    pool_scale,
    out_weight,
    mix_gain,
    expert_input,
    routes,
    route_weights,
    moe_in_gain,
    gate_weight,
    up_weight,
    down_weight,
    moe_out_gain,
):
    tp = lax.axis_index("tp")
    ep = lax.axis_index("ep")
    z, x, c = ep // (NX * NC), ep // NC % NX, ep % NC
    half = tp // 2
    tok = expert_input.shape[0]

    def mine(weight):
        return lax.dynamic_index_in_dim(weight, half, 0, keepdims=False)

    def others(weight):
        return lax.dynamic_index_in_dim(weight, 1 - half, 0, keepdims=False)

    gate_far = cross_swap(others(gate_weight))
    up_far = cross_swap(others(up_weight))
    down_far = cross_swap(others(down_weight))

    normed = rms_scale(expert_input.astype(F32), moe_in_gain).astype(BF)
    own_routes = lax.dynamic_slice_in_dim(routes, tp * tok, tok, 0)
    own_weights = lax.dynamic_slice_in_dim(route_weights, tp * tok, tok, 0)
    flat = own_routes.T.reshape(-1)
    pairs = flat.shape[0]
    earlier = lax.broadcasted_iota(jnp.int32, (pairs, pairs), 0) < lax.broadcasted_iota(
        jnp.int32, (pairs, pairs), 1
    )
    rank = jnp.sum(((flat[:, None] == flat[None, :]) & earlier).astype(jnp.int32), axis=0)
    home = flat // 2
    sz = (home // (NX * NC) - z) % NZ
    sx = (home // NC % NX - x) % NX
    sc = (home % NC) ^ c
    far = (flat % 2) ^ half
    slot = far * CHUNK + ((sx * NC + sc) * NZ + sz) * CAP + rank
    slot = slot.reshape(2, tok)
    lanes = lax.broadcasted_iota(jnp.int32, (2 * CHUNK, tok), 0)
    chosen = ((lanes == slot[0][None, :]) | (lanes == slot[1][None, :])).astype(BF)
    outgoing = dot32(chosen, normed).astype(BF)

    perm = perm_iota()
    arrived = []
    for so in range(2):
        crossed = []
        for q in range(NX * NC):
            piece = outgoing[so * CHUNK + q * MSG : so * CHUNK + (q + 1) * MSG]
            crossed.append(ep_shift(piece, 0, q // NC, q % NC))
        by_z = dot32(perm, jnp.concatenate(crossed, axis=0)).astype(BF)
        landed = [z_shift(by_z[s * MSG : (s + 1) * MSG], s, so == 1) for s in range(NZ)]
        arrived.append(jnp.concatenate(landed, axis=0))

    part_mix = mixer_start(pool_input, group_weight, pool_scale, out_weight, ep, tp)
    quarter = part_mix.shape[0] // NT

    gates = (mine(gate_weight), gate_far)
    ups = (mine(up_weight), up_far)
    downs = (mine(down_weight), down_far)
    summed = []
    for so in range(2):
        own = arrived[so]
        paired = pair_swap(own)
        parts = experts_on(jnp.concatenate([own, paired], axis=0), gates, ups, downs)
        back = pair_swap(parts[CHUNK:])
        summed.append((parts[:CHUNK].astype(F32) + back.astype(F32)).astype(BF))

    returned = []
    for so in range(2):
        crossed = [z_shift(summed[so][s * MSG : (s + 1) * MSG], -s, so == 1) for s in range(NZ)]
        by_q = dot32(perm, jnp.concatenate(crossed, axis=0)).astype(BF)
        for q in range(NX * NC):
            returned.append(ep_shift(by_q[q * MSG : (q + 1) * MSG], 0, -(q // NC), q % NC))
    returned = jnp.concatenate(returned, axis=0)

    lanes = lax.broadcasted_iota(jnp.int32, (tok, 2 * CHUNK), 1)
    spread = jnp.where(lanes == slot[0][:, None], own_weights[:, 0:1], 0.0) + jnp.where(
        lanes == slot[1][:, None], own_weights[:, 1:2], 0.0
    )
    high = spread.astype(BF)
    low = (spread - high.astype(F32)).astype(BF)
    combined = dot32(high, returned) + dot32(low, returned)
    moe_out = rms_scale(combined, moe_out_gain).astype(BF)

    first = pair_swap(part_mix[2 * quarter :])
    both = part_mix[: 2 * quarter].astype(F32) + first.astype(F32)
    second = cross_swap(both[quarter:].astype(BF))
    mixer_out = rms_scale(both[:quarter] + second.astype(F32), mix_gain).astype(BF)
    return (mixer_out, moe_out)


def solution(mesh):
    in_specs = (
        P("ep", "tp"),
        P("tp", None, None),
        P("tp"),
        P("tp", None),
        P(),
        P(("ep", "tp"), None),
        P("ep", None),
        P("ep", None),
        P(),
        P("ep", None, "tp"),
        P("ep", None, "tp"),
        P("ep", "tp", None),
        P(),
    )
    out_specs = (P(("ep", "tp"), None), P(("ep", "tp"), None))
    return jax.shard_map(
        on_device, mesh=mesh, in_specs=in_specs, out_specs=out_specs, check_vma=False
    )
```

```python
import jax
import jax.numpy as jnp
from jax import lax
from jax.experimental import pallas as pl
from jax.experimental.pallas import tpu as pltpu
from jax.sharding import PartitionSpec as P

NORM_EPS = 1e-06

NZ, NX, NC, NT = 8, 4, 2, 4
PLANE = NX * NC
CAP = 5
MSG = PLANE * CAP
CHUNK = NZ * MSG
BF = jnp.bfloat16
F32 = jnp.float32
OUT_PARTS = 4
HALVES = 2
Q_ORDER = (4, 5, 2, 3, 6, 7, 1, 0)
Z_ORDER = (4, 3, 5, 2, 6, 1, 7)

Q_GROUPS = [[z * PLANE + q for q in range(PLANE)] for z in range(NZ)]
Z_GROUPS = [[z * PLANE + q for z in range(NZ)] for q in range(PLANE)]


def sharer(t, c):
    return t ^ (1 + 2 * c)


def crosser(t, c):
    return t ^ (3 - 2 * c)


def permuted(value, move):
    pairs = []
    for z in range(NZ):
        for q in range(PLANE):
            for t in range(NT):
                nq, nt = move(q, t)
                pairs.append(((z * PLANE + q) * NT + t, (z * PLANE + nq) * NT + nt))
    return lax.ppermute(value, ("ep", "tp"), pairs)


def stepped(q, k, sign):
    x, c = divmod(q, NC)
    return (x + sign * (k // NC)) % NX * NC + (c + k) % NC


def out_shift(value, k):
    return permuted(value, lambda q, t: (stepped(q, k, 1), crosser(t, (q + k) % NC)))


def back_shift(value, k, far):
    if k == 0 and not far:
        return value
    return permuted(value, lambda q, t: (stepped(q, k, -1), crosser(t, q % NC) if far else t))


def z_shift(value, s):
    pairs = []
    for z in range(NZ):
        pairs += [(z * PLANE + q, (z + s) % NZ * PLANE + q) for q in range(PLANE)]
    return lax.ppermute(value, "ep", pairs)


def share_swap(value):
    return permuted(value, lambda q, t: (q, sharer(t, q % NC)))


def cross_swap(value):
    return permuted(value, lambda q, t: (q, crosser(t, q % NC)))


def exchange(value, groups):
    return lax.all_to_all(value, "ep", 0, 0, axis_index_groups=groups, tiled=True)


def rms_scale(values, gain_vec):
    mean_sq = jnp.mean(values * values, axis=-1, keepdims=True)
    return values * lax.rsqrt(mean_sq + NORM_EPS) * gain_vec


def dot32(a, b):
    return jnp.dot(a, b, preferred_element_type=F32)


def row_perm(q_of=None):
    i = lax.broadcasted_iota(jnp.int32, (CHUNK, 1), 0)
    j = lax.broadcasted_iota(jnp.int32, (CHUNK, CHUNK), 1)
    outer = i // MSG
    outer = outer if q_of is None else q_of(outer)
    source = (i % MSG // CAP * PLANE + outer) * CAP + i % CAP
    return (j == source).astype(F32).astype(BF)


def split_kernel(perm_ref, rows_ref, *out_refs):
    moved = dot32(perm_ref[...], rows_ref[...]).astype(BF)
    for s, out in enumerate(out_refs):
        out[...] = moved[s * MSG : (s + 1) * MSG]


def permute_and_split(perm, rows):
    width = rows.shape[-1]
    return pl.pallas_call(
        split_kernel,
        out_shape=[jax.ShapeDtypeStruct((MSG, width), BF)] * NZ,
        name="permute_and_split",
    )(perm, rows)


def join_permute_kernel(perm_ref, *refs):
    out, stage = refs[-2], refs[-1]
    for s in range(NZ):
        stage[s * MSG : (s + 1) * MSG, :] = refs[s][...]
    out[...] = dot32(perm_ref[...], stage[...]).astype(BF)


def join_and_permute(perm, pieces):
    width = pieces[0].shape[-1]
    return pl.pallas_call(
        join_permute_kernel,
        out_shape=jax.ShapeDtypeStruct((CHUNK, width), BF),
        scratch_shapes=[pltpu.VMEM((CHUNK, width), BF)],
        name="join_and_permute",
    )(perm, *pieces)


def summed(own_ref, half_refs):
    step = half_refs[0].shape[0]
    parts = [
        (own_ref[n * step : (n + 1) * step, :].astype(F32) + half[...].astype(F32)).astype(BF)
        for n, half in enumerate(half_refs)
    ]
    return jnp.concatenate(parts, axis=0)


def add_split_kernel(perm_ref, own_ref, *refs):
    moved = dot32(perm_ref[...], summed(own_ref, refs[:HALVES])).astype(BF)
    for s, out in enumerate(refs[HALVES:]):
        out[...] = moved[s * MSG : (s + 1) * MSG]


def add_and_split(perm, own, halves):
    width = own.shape[-1]
    return pl.pallas_call(
        add_split_kernel,
        out_shape=[jax.ShapeDtypeStruct((MSG, width), BF)] * NZ,
        name="add_and_split",
    )(perm, own, *halves)


def add_kernel(own_ref, *refs):
    refs[HALVES][...] = summed(own_ref, refs[:HALVES])


def add(own, halves):
    return pl.pallas_call(
        add_kernel, out_shape=jax.ShapeDtypeStruct(own.shape, BF), name="add"
    )(own, *halves)


def repack_kernel(perm_ref, *refs):
    stage = refs[-1]
    for s in range(NZ):
        stage[s * MSG : (s + 1) * MSG, :] = refs[s][...]
    moved = dot32(perm_ref[...], stage[...]).astype(BF)
    for s in range(PLANE):
        refs[NZ + s][...] = moved[s * MSG : (s + 1) * MSG]


def repack(perm, pieces):
    width = pieces[0].shape[-1]
    return pl.pallas_call(
        repack_kernel,
        out_shape=[jax.ShapeDtypeStruct((MSG, width), BF)] * PLANE,
        scratch_shapes=[pltpu.VMEM((CHUNK, width), BF)],
        name="repack",
    )(perm, *pieces)


def weighed(spread_ref, refs, stage):
    for s in range(NZ):
        stage[s * MSG : (s + 1) * MSG, :] = refs[s][...]
    spread = spread_ref[...]
    high = spread.astype(BF)
    low = (spread - high.astype(F32)).astype(BF)
    return dot32(high, stage[...]) + dot32(low, stage[...])


def combine_first_kernel(spread_ref, *refs):
    refs[-2][...] = weighed(spread_ref, refs, refs[-1])


def combine_last_kernel(spread_ref, gain_ref, first_ref, *refs):
    combined = first_ref[...] + weighed(spread_ref, refs, refs[-1])
    refs[-2][...] = rms_scale(combined, gain_ref[...]).astype(BF)


def combine(kernel, kind, spread, extras, pieces):
    width = pieces[0].shape[-1]
    return pl.pallas_call(
        kernel,
        out_shape=jax.ShapeDtypeStruct((spread.shape[0], width), kind),
        scratch_shapes=[pltpu.VMEM((CHUNK, width), BF)],
        compiler_params=pltpu.CompilerParams(vmem_limit_bytes=32 * 2**20),
    )(spread, *extras, *pieces)


def pack_kernel(half_ref, gate_ref, up_ref, down_ref, out_ref, stage, sems, out_sems):
    other = 1 - half_ref[0]
    width, units = gate_ref.shape[1:]
    sources = [(gate_ref.at[other], 0, width), (up_ref.at[other], width, width)]
    for n in range(width // units):
        block = down_ref.at[other, :, pl.ds(n * units, units)]
        sources.append((block, 2 * width + n * units, units))
    reads, writes = [], []
    for n, (source, first, count) in enumerate(sources):
        rows = pl.ds(first, count)
        reads.append(pltpu.make_async_copy(source, stage.at[rows], sems.at[n]))
        writes.append(pltpu.make_async_copy(stage.at[rows], out_ref.at[rows], out_sems.at[n]))
    for read in reads:
        read.start()
    for read, write in zip(reads, writes):
        read.wait()
        write.start()
    for write in writes:
        write.wait()


def pack_weights(half, own):
    width, units = own[0].shape[1:]
    hbm = pl.BlockSpec(memory_space=pltpu.HBM)
    pieces = 2 + width // units
    return pl.pallas_call(
        pack_kernel,
        out_shape=jax.ShapeDtypeStruct((3 * width, units), BF),
        in_specs=[pl.BlockSpec(memory_space=pltpu.SMEM)] + [hbm] * 3,
        out_specs=hbm,
        scratch_shapes=[
            pltpu.VMEM((3 * width, units), BF),
            pltpu.SemaphoreType.DMA((pieces,)),
            pltpu.SemaphoreType.DMA((pieces,)),
        ],
        name="pack_weights",
    )(half, *own)


def expert_kernel(
    half_ref, rows_ref, gate_ref, up_ref, down_ref, far_ref,
    out_ref, rows, result, gates, ups, downs, sems, out_sems,
):
    width, units = gates.shape[1:]
    half = half_ref[0]
    sources = (
        (rows_ref, rows),
        (gate_ref.at[half], gates.at[0]),
        (up_ref.at[half], ups.at[0]),
        (far_ref.at[pl.ds(0, width)], gates.at[1]),
        (far_ref.at[pl.ds(width, width)], ups.at[1]),
        (down_ref.at[half], downs.at[0]),
    )
    copies = [pltpu.make_async_copy(a, b, sems.at[n]) for n, (a, b) in enumerate(sources)]
    for n in range(width // units):
        copies.append(
            pltpu.make_async_copy(
                far_ref.at[pl.ds(2 * width + n * units, units)],
                downs.at[1, :, pl.ds(n * units, units)],
                sems.at[6 + n],
            )
        )
    for copy in copies:
        copy.start()
    copies[0].wait()
    hidden = []
    for b in range(2):
        copies[1 + 2 * b].wait()
        gate = dot32(rows[...], gates[b])
        copies[2 + 2 * b].wait()
        up = dot32(rows[...], ups[b])
        hidden.append((gate / (1.0 + jnp.exp(-gate)) * up).astype(BF))
    for copy in copies[5:]:
        copy.wait()
    step = width // OUT_PARTS
    sends = []
    for n in range(OUT_PARTS):
        cols = slice(n * step, (n + 1) * step)
        result[:, cols] = (
            dot32(hidden[0], downs[0, :, cols]) + dot32(hidden[1], downs[1, :, cols])
        ).astype(BF)
        sends.append(
            pltpu.make_async_copy(result.at[:, cols], out_ref.at[:, cols], out_sems.at[n])
        )
        sends[-1].start()
    for send in sends:
        send.wait()


def experts_on(half, rows, own, far):
    width = rows.shape[-1]
    units = far.shape[-1]
    hbm = pl.BlockSpec(memory_space=pltpu.HBM)
    flops = 6 * rows.shape[0] * width * 2 * units
    return pl.pallas_call(
        expert_kernel,
        out_shape=jax.ShapeDtypeStruct(rows.shape, BF),
        in_specs=[pl.BlockSpec(memory_space=pltpu.SMEM)] + [hbm] * 5,
        out_specs=hbm,
        scratch_shapes=[
            pltpu.VMEM(rows.shape, BF),
            pltpu.VMEM(rows.shape, BF),
            pltpu.VMEM((2, width, units), BF),
            pltpu.VMEM((2, width, units), BF),
            pltpu.VMEM((2, units, width), BF),
            pltpu.SemaphoreType.DMA((6 + width // units,)),
            pltpu.SemaphoreType.DMA((OUT_PARTS,)),
        ],
        cost_estimate=pl.CostEstimate(
            flops=flops, bytes_accessed=4 * rows.size + 12 * width * units, transcendentals=0
        ),
        compiler_params=pltpu.CompilerParams(vmem_limit_bytes=60 * 2**20),
        name="experts",
    )(half, rows, *own, far)


def mixer_start(history, pool_input, group_weight, pool_scale, out_weight, ep, tp, c):
    rows = pool_input.shape[0]
    hist = history.shape[0]
    quarter = rows // NT
    window = jnp.left_shift(jnp.int32(2), tp)
    extended = jnp.concatenate([history, pool_input], axis=0)
    line = lax.broadcasted_iota(jnp.int32, (rows, 1), 0)
    block = line // quarter
    owner = tp ^ jnp.where(block % 2 == 0, 0, 3 - 2 * c) ^ jnp.where(block < 2, 0, 1 + 2 * c)
    place = owner * quarter + line % quarter
    source = lax.broadcasted_iota(jnp.int32, (rows, rows + hist), 1) - hist
    band = ((source <= place) & (source > place - window)).astype(BF)
    pick = (source == place).astype(BF)
    divisor = jnp.minimum(ep * rows + place + 1, window).astype(F32)
    pooled = (dot32(band, extended) / divisor - dot32(pick, extended)).astype(BF)
    grouped = (dot32(pooled, group_weight[0]) * pool_scale).astype(BF)
    return dot32(grouped, out_weight).astype(BF)


def on_device(
    pool_input,
    group_weight,
    pool_scale,
    out_weight,
    mix_gain,
    expert_input,
    routes,
    route_weights,
    moe_in_gain,
    gate_weight,
    up_weight,
    down_weight,
    moe_out_gain,
):
    tp = lax.axis_index("tp")
    ep = lax.axis_index("ep")
    c = ep % NC
    half = (tp + c) // 2 % 2
    half_ref = half.reshape(1)
    tok, _ = expert_input.shape

    own = (gate_weight, up_weight, down_weight)
    far = pack_weights(half_ref, own)
    far, expert_input = lax.optimization_barrier((far, expert_input))
    far = cross_swap(far)

    normed = rms_scale(expert_input.astype(F32), moe_in_gain).astype(BF)
    own_routes = lax.dynamic_slice_in_dim(routes, tp * tok, tok, 0)
    own_weights = lax.dynamic_slice_in_dim(route_weights, tp * tok, tok, 0)
    flat = own_routes.T.reshape(-1)
    pairs = flat.shape[0]
    earlier = lax.broadcasted_iota(jnp.int32, (pairs, pairs), 0) < lax.broadcasted_iota(
        jnp.int32, (pairs, pairs), 1
    )
    rank = jnp.sum(((flat[:, None] == flat[None, :]) & earlier).astype(jnp.int32), axis=0)
    home = flat // 2
    crossing = flat % 2 ^ (tp + home % NC) // 2 % 2
    x = ep // NC % NX
    there, level = home % PLANE, home // PLANE
    level = jnp.where(crossing == 1, level, (level - ep // PLANE) % NZ)
    step = (there // NC - x) % NX * NC + (there + c) % NC
    slot_back = (crossing * CHUNK + step * MSG + level * CAP + rank).reshape(2, tok)
    slot = jnp.where(crossing == 1, slot_back.reshape(-1), level * MSG + there * CAP + rank)
    slot = slot.reshape(2, tok)
    lanes = lax.broadcasted_iota(jnp.int32, (2 * CHUNK, tok), 0)
    chosen = ((lanes == slot[0][None, :]) | (lanes == slot[1][None, :])).astype(BF)
    outgoing = dot32(chosen, normed).astype(BF)

    perm = row_perm()
    perm_near = row_perm(lambda k: (x - k // NC) % NX * NC + (k + c) % NC)

    near = [outgoing[k * MSG : (k + 1) * MSG] for k in range(NZ)]
    for k in Z_ORDER:
        near[k] = z_shift(near[k], k)
    pieces = [None] * PLANE
    for k in Q_ORDER:
        first_row = CHUNK + k * MSG
        pieces[k] = out_shift(outgoing[first_row : first_row + MSG], k)
    ends = pool_input[pool_input.shape[0] - 2**NT :]
    history = lax.ppermute(ends, "ep", [(e, e + 1) for e in range(NZ * PLANE - 1)])
    near = join_and_permute(perm, near)
    near = exchange(near, Q_GROUPS)
    by_z = join_and_permute(perm, pieces)
    distant = exchange(by_z, Z_GROUPS)

    results = []
    for so, rows in zip("SO", (near, distant)):
        step = CHUNK // HALVES
        paired = []
        for n in range(HALVES):
            paired.append(share_swap(rows[n * step : (n + 1) * step]))
        mine = experts_on(half_ref, rows, own, far)
        back = []
        for n in range(HALVES):
            theirs = experts_on(half_ref, paired[n], own, far)
            back.append(share_swap(theirs))
        results.append(list(add_and_split(perm, mine, back)) if so == "S" else add(mine, back))

    lanes = lax.broadcasted_iota(jnp.int32, (tok, 2 * CHUNK), 1)
    spread = jnp.where(lanes == slot_back[0][:, None], own_weights[:, 0:1], 0.0) + jnp.where(
        lanes == slot_back[1][:, None], own_weights[:, 1:2], 0.0
    )
    home_near, home_far = results
    history, home_far = lax.optimization_barrier((history, home_far))
    part_mix = mixer_start(history, pool_input, group_weight, pool_scale, out_weight, ep, tp, c)
    quarter = part_mix.shape[0] // NT
    first = share_swap(part_mix[2 * quarter :])
    both = part_mix[: 2 * quarter].astype(F32) + first.astype(F32)
    second = cross_swap(both[quarter:].astype(BF))
    mixer_out = rms_scale(both[:quarter] + second.astype(F32), mix_gain).astype(BF)

    for k in Z_ORDER:
        home_near[k] = z_shift(home_near[k], -k)
    home_far = exchange(home_far, Z_GROUPS)
    returned = []
    for so in "SO":
        if so == "S":
            pieces = list(repack(perm_near, home_near))
        else:
            pieces = list(permute_and_split(perm, home_far))
        for k in Q_ORDER:
            pieces[k] = back_shift(pieces[k], k, so == "O")
        returned.append(pieces)
    combined = combine(combine_first_kernel, F32, spread[:, :CHUNK], (), returned[0])
    moe_out = combine(
        combine_last_kernel, BF, spread[:, CHUNK:], (moe_out_gain[None], combined), returned[1]
    )
    return (mixer_out, moe_out)


def solution(mesh):
    in_specs = (
        P("ep", "tp"),
        P("tp", None, None),
        P("tp"),
        P("tp", None),
        P(),
        P(("ep", "tp"), None),
        P("ep", None),
        P("ep", None),
        P(),
        P("ep", None, "tp"),
        P("ep", None, "tp"),
        P("ep", "tp", None),
        P(),
    )
    out_specs = (P(("ep", "tp"), None), P(("ep", "tp"), None))
    return jax.shard_map(
        on_device, mesh=mesh, in_specs=in_specs, out_specs=out_specs, check_vma=False
    )
```
